256 devices in a mesh: grp: 2 (over y), sp: 32 (over z, core), tp: 4 (over x).
Axes of the slice: x: 4, y: 2, z: 16, core: 2. Of those that a mesh axis runs over, the one named last changes fastest.
The devices are a block of a 4x16x16 slice.
Arguments:
- stream: bfloat16 [32768, 2048], P(('grp', 'sp')), parts along dimension 0, may hold values from -6 to 6
- queries_a: bfloat16 [32768, 512], P(('grp', 'sp'), 'tp'), parts along dimension 0, may hold values from -6 to 6
- keys_a: bfloat16 [32768, 512], P(('grp', 'sp'), 'tp'), parts along dimension 0, may hold values from -6 to 6
- queries_b: bfloat16 [32768, 1024], P(('grp', 'sp'), 'tp'), parts along dimension 0, may hold values from -6 to 6
- keys_b: bfloat16 [32768, 1024], P(('grp', 'sp'), 'tp'), parts along dimension 0, may hold values from -6 to 6
- values: bfloat16 [32768, 2, 1024], P(('grp', 'sp'), None, 'tp'), parts along dimension 0, may hold values from -6 to 6
- out_gate: bfloat16 [32768, 2, 1024], P(('grp', 'sp'), None, 'tp'), parts along dimension 0, may hold values from -6 to 6
- in_gate: float32 [2, 8, 32768], P(None, 'tp', ('grp', 'sp')), parts along dimension 2, may hold values from -4 to 250
- forget_gate: float32 [2, 8, 32768], P(None, 'tp', ('grp', 'sp')), parts along dimension 2, may hold values from -5 to 16
- head_gain: float32 [2, 1024], P(None, 'tp'), may hold values from 0.1 to 1.9
- out_weight: bfloat16 [2, 1024, 2048], P(None, 'tp'), may hold values from -0.125 to 0.125
- norm_gain: float32 [2048], replicated, may hold values from 0.1 to 1.9
- gate_weight: bfloat16 [2048, 5632], P('sp', 'tp'), may hold values from -0.125 to 0.125
- up_weight: bfloat16 [2048, 5632], P('sp', 'tp'), may hold values from -0.125 to 0.125
- down_weight: bfloat16 [5632, 2048], P('tp', 'sp'), may hold values from -0.078125 to 0.078125
Outputs:
- layer_out: bfloat16 [32768, 2048], P(('grp', 'sp', 'tp')), parts along dimension 0
The draws below stay inside these ranges and needn't reach their ends.
There are 2 independent parts, one for each index of `grp`. The reference program is written for one: setup_inputs(seed, part) draws one part's arguments, and reference() takes and returns one part's arrays. A program takes and returns all parts, laid end to end along the dimension named above; an argument that names none is the same for every part. Nothing has to cross between parts.
All inputs are finite; a program needn't handle non-finite values.
Results may differ from the reference program's by a relative error of at most 0.013.
Values may be sent and summed in bfloat16 or wider, within the bound.
A program may use at most 128 MiB of HBM per device.

```python
import math
import jax
import jax.numpy as jnp
from jax import lax

D = 2048
HALF = 8
DKA = 64
DKB = 128
DV = 128
FF = 5632
TOK_DEV = 512
SEQUENCE_TOKENS = 16384
N_TP = 4


def draw_forget_gate(key, part):
    key_rows = jax.random.split(jax.random.fold_in(key, 17), 7)
    tensor_dims = (2, HALF, SEQUENCE_TOKENS)
    slow_share = 0.5
    slow = jax.random.uniform(key_rows[0], (2, HALF, 1)) < slow_share
    slow_rate = jnp.exp(jax.random.uniform(key_rows[1], (2, HALF, 1), minval=math.log(0.1), maxval=math.log(0.4))) / SEQUENCE_TOKENS
    span = jnp.exp(jax.random.uniform(key_rows[2], (2, HALF, 1), minval=math.log(max(TOK_DEV / 16, 2.0)), maxval=math.log(max(TOK_DEV / 5, 4.0))))
    rate = jnp.where(slow, slow_rate, 1.0 / span)
    factor = jnp.exp(jax.random.uniform(key_rows[3], (2, HALF, SEQUENCE_TOKENS // TOK_DEV), minval=0.0, maxval=math.log(4.0)))
    rate = rate * jnp.repeat(factor, TOK_DEV, axis=2)
    noise = jnp.clip(0.7 * jax.random.normal(key_rows[4], tensor_dims), -2.5, 2.5)
    preactivation = -jnp.log(jnp.expm1(rate)) + noise
    gate_spike = jax.random.uniform(key_rows[5], tensor_dims) < 3.0 / SEQUENCE_TOKENS
    retained_rows = jax.random.uniform(key_rows[6], tensor_dims, minval=0.5, maxval=0.8)
    return jnp.where(gate_spike, jnp.log(retained_rows / (1.0 - retained_rows)), preactivation).astype(jnp.float32)


def draw_in_gate(key, part):
    key_rows = jax.random.split(jax.random.fold_in(key, 23), 1)
    tensor_dims = (2, HALF, SEQUENCE_TOKENS)
    base = jnp.clip(jax.random.normal(key_rows[0], tensor_dims), -4.0, 4.0)
    return base.astype(jnp.float32)


def shard_levels(key, shape, cuts, low, largest):
    def one(position, parts):
        heights = jax.random.uniform(jax.random.fold_in(jax.random.fold_in(key, 6), position), (parts,), jnp.float32, low / len(cuts), largest / len(cuts))
        return jnp.repeat(jnp.exp(heights), shape[position] // parts).reshape((-1,) + (1,) * (len(shape) - position - 1))

    loudness = one(*cuts[0])
    for cut in cuts[1:]:
        loudness = loudness * one(*cut)
    return loudness


def bell_draw(key, shape, deviation, bound, cuts=(), kind=jnp.bfloat16):
    values = jax.random.normal(key, shape, jnp.float32) * deviation
    if len(cuts) > 0:
        values = shard_levels(key, shape, cuts, -0.22, 0.18) * values
    return jnp.clip(values, min=-bound, max=bound).astype(kind)


def setup_inputs(seed: int = 0, part: int = 0) -> dict:
    seeds = jax.random.split(jax.random.key(seed), 16)
    part_splits = jax.random.split(jax.random.fold_in(seeds[15], part), 16)
    return {
        "stream": bell_draw(part_splits[0], (SEQUENCE_TOKENS, D), 1.0, 6.0, ((0, 32),)),
        "queries_a": bell_draw(part_splits[1], (SEQUENCE_TOKENS, HALF * DKA), 1.0, 6.0, ((0, 32), (1, 4))),
        "keys_a": bell_draw(part_splits[2], (SEQUENCE_TOKENS, HALF * DKA), 1.0, 6.0, ((0, 32), (1, 4))),
        "queries_b": bell_draw(part_splits[3], (SEQUENCE_TOKENS, HALF * DKB), 1.0, 6.0, ((0, 32), (1, 4))),
        "keys_b": bell_draw(part_splits[4], (SEQUENCE_TOKENS, HALF * DKB), 1.0, 6.0, ((0, 32), (1, 4))),
        "values": bell_draw(part_splits[5], (SEQUENCE_TOKENS, 2, HALF * DV), 1.0, 6.0, ((0, 32), (2, 4))),
        "out_gate": bell_draw(part_splits[6], (SEQUENCE_TOKENS, 2, HALF * DV), 1.5, 6.0, ((0, 32), (2, 4))),
        "in_gate": draw_in_gate(jax.random.fold_in(jax.random.fold_in(seeds[15], part), 71), part),
        "forget_gate": draw_forget_gate(jax.random.fold_in(jax.random.fold_in(seeds[15], part), 71), part),
        "head_gain": jnp.clip(1.0 + 0.18 * jax.random.normal(seeds[9], (2, HALF * DV), jnp.float32), 0.1, 1.9),
        "out_weight": bell_draw(seeds[10], (2, HALF * DV, D), (2 * HALF * DV) ** -0.5, 0.125, ((1, 4),)),
        "norm_gain": jnp.clip(1.0 + 0.18 * jax.random.normal(seeds[11], (D,), jnp.float32), 0.1, 1.9),
        "gate_weight": bell_draw(seeds[12], (D, FF), D ** -0.5, 0.125, ((0, 32), (1, 4))),
        "up_weight": bell_draw(seeds[13], (D, FF), D ** -0.5, 0.125, ((0, 32), (1, 4))),
        "down_weight": bell_draw(seeds[14], (FF, D), FF ** -0.5, 0.078125, ((0, 4), (1, 32))),
    }


EPS = 1e-06
NEG = -1e+30
HIGHEST = lax.Precision.HIGHEST

def rounded(partial_value):
    return lax.optimization_barrier(partial_value.astype(jnp.bfloat16)).astype(jnp.float32)

def block_state(key_rows, values, in_rates, forget_rates):
    cumul = jnp.cumsum(jax.nn.log_sigmoid(forget_rates), axis=1)
    total = cumul[:, -1]
    tail = total[:, None] - cumul + in_rates
    peak = lax.optimization_barrier(jnp.max(tail, axis=1))
    weight = jnp.exp(tail - peak[:, None])
    weighted = rounded(values.astype(jnp.float32) * jnp.transpose(weight)[:, :, None])
    keys_wide = key_rows.astype(jnp.float32)
    state = jnp.einsum('rhv,rhk->hvk', weighted, keys_wide, precision=HIGHEST)
    norm_vec = jnp.einsum('hr,rhk->hk', weight, keys_wide, precision=HIGHEST)
    return ((state, norm_vec, peak, total), cumul)

def read_block(queries, key_rows, values, in_rates, cumul, carried, scale):
    length = queries.shape[0]
    query_wide = queries.astype(jnp.float32)
    scores = jnp.einsum('rhk,shk->hrs', query_wide, key_rows.astype(jnp.float32), precision=HIGHEST) * scale
    causal = lax.broadcasted_iota(jnp.int32, (length, length), 0) >= lax.broadcasted_iota(jnp.int32, (length, length), 1)
    decay_log = cumul[:, :, None] - cumul[:, None, :] + in_rates[:, None, :]
    decay_log = jnp.where(causal[None], decay_log, -jnp.inf)
    carried_log = cumul + carried[2][:, None]
    stabil = jnp.maximum(carried_log, lax.optimization_barrier(jnp.max(decay_log, axis=2)))
    weight_matrices = scores * jnp.exp(decay_log - stabil[:, :, None])
    carried_weight = jnp.exp(carried_log - stabil) * scale
    denom = lax.optimization_barrier(jnp.sum(weight_matrices, axis=2)) + carried_weight * jnp.einsum('hk,rhk->hr', carried[1], query_wide, precision=HIGHEST)
    numer = jnp.einsum('hrs,shv->rhv', rounded(weight_matrices), values.astype(jnp.float32), precision=HIGHEST)
    numer = numer + jnp.transpose(carried_weight)[:, :, None] * jnp.einsum('hvk,rhk->rhv', carried[0], query_wide, precision=HIGHEST)
    floor_val = jnp.maximum(jnp.abs(denom), jnp.exp(-stabil))
    return numer / jnp.transpose(floor_val)[:, :, None]

def combine_group(earlier, later):
    peak = jnp.maximum(later[3] + earlier[2], later[2])
    initial_scale = jnp.exp(later[3] + earlier[2] - peak)
    late_scale = jnp.exp(later[2] - peak)
    state = initial_scale[:, None, None] * earlier[0] + late_scale[:, None, None] * later[0]
    norm_vec = initial_scale[:, None] * earlier[1] + late_scale[:, None] * later[1]
    return (state, norm_vec, peak, earlier[3] + later[3])

def mixer_group(queries, key_rows, values, in_rates, forget_rates):
    key_size = queries.shape[1] // HALF
    blocks = SEQUENCE_TOKENS // TOK_DEV
    scale = key_size ** (-0.5)
    query_blocks = queries.reshape(blocks, TOK_DEV, HALF, key_size)
    key_blocks = key_rows.reshape(blocks, TOK_DEV, HALF, key_size)
    value_blocks = values.reshape(blocks, TOK_DEV, HALF, DV)
    in_blocks = jnp.transpose(in_rates.reshape(HALF, blocks, TOK_DEV), (1, 0, 2))
    forget_blocks = jnp.transpose(forget_rates.reshape(HALF, blocks, TOK_DEV), (1, 0, 2))

    def advance(carried, pieces):
        query_block, key_block, value_block, in_block, forget_block = pieces
        own, cumul = block_state(key_block, value_block, in_block, forget_block)
        cell = read_block(query_block, key_block, value_block, in_block, cumul, carried, scale)
        return (combine_group(carried, own), cell)
    start_state = (jnp.zeros((HALF, DV, key_size), jnp.float32), jnp.zeros((HALF, key_size), jnp.float32), jnp.full((HALF,), NEG, jnp.float32), jnp.zeros((HALF,), jnp.float32))
    _, cells = lax.scan(advance, start_state, (query_blocks, key_blocks, value_blocks, in_blocks, forget_blocks))
    return cells.reshape(SEQUENCE_TOKENS, HALF, DV)

def head_output(cell, gain, gate):
    lines = cell.shape[0]
    normed = cell * lax.rsqrt(lax.optimization_barrier(jnp.mean(cell * cell, axis=(1, 2), keepdims=True)) + EPS)
    return (normed.reshape(lines, -1) * gain * jax.nn.sigmoid(gate.astype(jnp.float32))).astype(jnp.bfloat16)

def reference(stream, queries_a, keys_a, queries_b, keys_b, values, out_gate, in_gate, forget_gate, head_gain, out_weight, norm_gain, gate_weight, up_weight, down_weight):
    mixed_first = head_output(mixer_group(queries_a, keys_a, values[:, 0], in_gate[0], forget_gate[0]), head_gain[0], out_gate[:, 0])
    mixed_second = head_output(mixer_group(queries_b, keys_b, values[:, 1], in_gate[1], forget_gate[1]), head_gain[1], out_gate[:, 1])
    width = HALF * DV // N_TP
    mixture = jnp.zeros((SEQUENCE_TOKENS, D), jnp.float32)
    for part_index in range(N_TP):
        cols = slice(part_index * width, (part_index + 1) * width)
        partial_value = jnp.dot(mixed_first[:, cols], out_weight[0, cols], preferred_element_type=jnp.float32)
        partial_value = partial_value + jnp.dot(mixed_second[:, cols], out_weight[1, cols], preferred_element_type=jnp.float32)
        mixture = mixture + rounded(partial_value)
    residual = stream.astype(jnp.float32) + mixture
    normed = (residual * lax.rsqrt(lax.optimization_barrier(jnp.mean(residual * residual, axis=1, keepdims=True)) + EPS) * norm_gain).astype(jnp.bfloat16)
    gate = jnp.dot(normed, gate_weight, preferred_element_type=jnp.float32)
    up_proj = jnp.dot(normed, up_weight, preferred_element_type=jnp.float32)
    active = (jax.nn.silu(gate) * up_proj).astype(jnp.bfloat16)
    hidden_part = FF // N_TP
    result = residual
    for part_index in range(N_TP):
        units = slice(part_index * hidden_part, (part_index + 1) * hidden_part)
        result = result + rounded(jnp.dot(active[:, units], down_weight[units], preferred_element_type=jnp.float32))
    return result.astype(jnp.bfloat16)
```

```python
import functools

import jax
import jax.numpy as jnp
from jax import lax
from jax.experimental import pallas as pl
from jax.experimental.pallas import tpu as pltpu
from jax.sharding import PartitionSpec as P

F32 = jnp.float32
BF16 = jnp.bfloat16
HIGHEST = lax.Precision.HIGHEST
EPS = 1e-06
NEG = -1e30
LANES = 128
PIECE = 16
INTERPRET = False


def iota(shape, dim):
    return lax.broadcasted_iota(jnp.int32, shape, dim)


def dot(a, b, ca=1, cb=0, precision=None):
    return lax.dot_general(
        a, b, (((ca,), (cb,)), ((), ())), preferred_element_type=F32, precision=precision
    )


def call(kernel, name, out_shape, flops, nbytes, scratch=(), **kw):
    return pl.pallas_call(
        kernel,
        name=name,
        out_shape=out_shape,
        scratch_shapes=scratch,
        interpret=INTERPRET,
        cost_estimate=pl.CostEstimate(flops=flops, bytes_accessed=nbytes, transcendentals=0),
        **kw,
    )


def sds(shape, dtype):
    return jax.ShapeDtypeStruct(shape, dtype)


def state_kernel(ka_ref, kb_ref, v_ref, in_ref, forget_ref, out_ref, cum_ref, held):
    length = ka_ref.shape[0]
    f = forget_ref[...]
    ls = jnp.minimum(f, 0.0) - jnp.log1p(jnp.exp(-jnp.abs(f)))
    upto = (iota((length, length), 0) <= iota((length, length), 1)).astype(F32)
    cum = dot(ls, upto, precision=HIGHEST)
    cum_ref[...] = cum
    total = cum[:, length - 1 : length]
    tail = total - cum + in_ref[...]
    peak = jnp.max(tail, axis=1, keepdims=True)
    weight = jnp.exp(tail - peak)
    by_row = jnp.transpose(weight)
    first = iota((LANES, LANES), 1) < LANES // 2
    first_row = iota((1, LANES), 1) < LANES // 2
    ka = ka_ref[...]

    def weighted(n):
        v = v_ref[:, n * LANES : (n + 1) * LANES].astype(F32)
        return (v * by_row[:, n : n + 1]).astype(BF16)

    held[0] = jnp.where(first, dot(weighted(0), ka, 0, 0), dot(weighted(1), ka, 0, 0))
    na = dot(weight, ka.astype(F32), precision=HIGHEST)
    norms = [jnp.where(first_row, na[0:1], na[1:2])]
    for h in range(2):
        kb = kb_ref[:, h * LANES : (h + 1) * LANES]
        held[1 + h] = dot(weighted(2 + h), kb, 0, 0)
        norms.append(dot(weight, kb.astype(F32), precision=HIGHEST)[2 + h : 3 + h])
    row, lane = iota((8, LANES), 0), iota((8, LANES), 1)
    scalars = jnp.where(lane == row, total, 0.0) + jnp.where(lane == row + 8, peak, 0.0)
    norms.append(jnp.sum(scalars, axis=0, keepdims=True))
    last = jnp.concatenate(norms, axis=0)
    for j in range(out_ref.shape[0]):
        for m in range(3):
            out_ref[j, 4 * m : 4 * m + 4, :] = held[m, 4 * j : 4 * j + 4, :]
        out_ref[j, 12:16, :] = last


def fold_kernel(r_ref, o_ref, w_ref):
    n = r_ref.shape[0]
    scalars = jnp.transpose(r_ref[:, 15, :])
    e, a = scalars[0:8], scalars[8:16]
    j = iota((8, n), 1)
    row, lane = iota((8, LANES), 0), iota((8, LANES), 1)
    gap = jnp.zeros((8, n), F32)
    for i in range(n):
        if i == 0:
            peak = jnp.full((8, 1), NEG, F32)
            w_ref[i] = jnp.zeros((8, n), F32)
        else:
            gap = jnp.where(j < i - 1, gap + e[:, i - 1 : i], 0.0)
            level = jnp.where(j < i, gap + a, -jnp.inf)
            peak = jnp.maximum(jnp.max(level, axis=1, keepdims=True), NEG)
            w_ref[i] = jnp.exp(level - peak)
        o_ref[i, 15:16, :] = jnp.sum(jnp.where(lane == row, peak, 0.0), axis=0, keepdims=True)
    first = iota((n, 5 * LANES), 1) % LANES < LANES // 2
    for m in range(3):
        rows = [4 * m, 4 * m + 1, 4 * m + 2, 4 * m + 3, 12 + m]
        x = jnp.concatenate([r_ref[:, r, :] for r in rows], axis=1)
        if m == 0:
            y = jnp.where(
                first,
                dot(w_ref[:, 0, :], x, precision=HIGHEST),
                dot(w_ref[:, 1, :], x, precision=HIGHEST),
            )
        else:
            y = dot(w_ref[:, 1 + m, :], x, precision=HIGHEST)
        for k, r in enumerate(rows):
            o_ref[:, r, :] = y[:, k * LANES : (k + 1) * LANES]


def read_kernel(
    scales,
    qa_ref,
    ka_ref,
    qb_ref,
    kb_ref,
    v_ref,
    gate_ref,
    gain_ref,
    in_ref,
    cum_ref,
    p_ref,
    y_ref,
    held,
):
    length = qa_ref.shape[0]
    rows = 128
    for j in range(p_ref.shape[0]):
        for m in range(3):
            held[m, 4 * j : 4 * j + 4, :] = p_ref[j, 4 * m : 4 * m + 4, :]
    cum_col = jnp.transpose(cum_ref[...])
    lane_half = iota((rows, LANES), 1) < LANES // 2
    states = []
    for m in range(3):
        state = held[m]
        high = state.astype(BF16)
        states.append((high, (state - high.astype(F32)).astype(BF16)))
    for at in range(0, length, rows):
        seen = at + rows
        causal = iota((rows, seen), 0) + at >= iota((rows, seen), 1)
        squares = []
        for group in range(2):
            square = None
            for h in range(2):
                n = 2 * group + h
                m = 0 if group == 0 else 1 + h
                if group == 0:
                    q = qa_ref[at : at + rows, :]
                    q = jnp.where(lane_half == (h == 0), q, jnp.zeros_like(q))
                    k = ka_ref[0:seen, :]
                else:
                    q = qb_ref[at : at + rows, h * LANES : (h + 1) * LANES]
                    k = kb_ref[0:seen, h * LANES : (h + 1) * LANES]
                scale = scales[group]
                start = p_ref[0, 15:16, n : n + 1]
                c = cum_col[at : at + rows, n : n + 1]
                level = c - cum_ref[n : n + 1, 0:seen] + in_ref[n : n + 1, 0:seen]
                level = jnp.where(causal, level, -jnp.inf)
                carried = c + start
                peak = jnp.maximum(carried, jnp.max(level, axis=1, keepdims=True))
                p = dot(q, k, 1, 1) * scale * jnp.exp(level - peak)
                before = jnp.exp(carried - peak) * scale
                reach = jnp.sum(q.astype(F32) * p_ref[0, 12 + m : 13 + m, :], axis=1, keepdims=True)
                den = jnp.sum(p, axis=1, keepdims=True) + before * reach
                v = v_ref[0:seen, n * LANES : (n + 1) * LANES]
                high, low = states[m]
                num = dot(p.astype(BF16), v) + before * (dot(q, high, 1, 1) + dot(q, low, 1, 1))
                cell = num / jnp.maximum(jnp.abs(den), jnp.exp(-peak))
                part = jnp.sum(cell * cell, axis=1, keepdims=True)
                square = part if square is None else square + part
                columns = slice(n * LANES, (n + 1) * LANES)
                gate = gate_ref[at : at + rows, columns].astype(F32)
                y = cell * gain_ref[0:1, columns] / (1.0 + jnp.exp(-gate))
                y_ref[at : at + rows, columns] = y.astype(BF16)
            squares.append(square)
        lane = iota((rows, LANES), 1)
        extra = jnp.zeros((rows, LANES), F32)
        for group in range(2):
            left = squares[group]
            for k in range(3):
                piece = left.astype(BF16).astype(F32)
                extra = jnp.where(lane == 3 * group + k, piece, extra)
                left = left - piece
        y_ref[at : at + rows, 4 * LANES :] = extra.astype(BF16)


def project_kernel(
    where_ref, y_ref, own_ref, *refs
):
    tp, rows, _ = y_ref.shape
    mine_refs, other_refs = refs[0 : tp - 1], refs[tp - 1 : 2 * tp - 2]
    stream_ref, gain_ref, res_ref, out_ref = refs[2 * tp - 2 :]
    step = pl.program_id(0)
    width = own_ref.shape[2]
    half = own_ref.shape[1]
    me, core = where_ref[0], where_ref[1]
    total = jnp.zeros((rows, LANES), F32)
    for j in range(tp):
        total = total + y_ref[j, :, 2 * half :].astype(F32)
    group_columns = tp * half
    norms = []
    for g in range(2):
        square = jnp.sum(total[:, 3 * g : 3 * g + 3], axis=1, keepdims=True)
        norms.append(lax.rsqrt(square / group_columns + EPS))
    y = y_ref[me]
    sums = [dot(y[:, g * half : (g + 1) * half], own_ref[g]) for g in range(2)]
    even = core == 0
    same = jnp.zeros((rows, width), F32)
    cross = jnp.zeros((rows, width), F32)
    for d in range(1, tp):
        y = y_ref[lax.rem(me + d, tp)]
        first, second = y[:, 0:half], y[:, half : 2 * half]
        same = same + dot(jnp.where(even, first, second), mine_refs[d - 1][...])
        cross = cross + dot(jnp.where(even, second, first), other_refs[d - 1][...])
    mix = norms[0] * (sums[0] + jnp.where(even, same, cross))
    mix = mix + norms[1] * (sums[1] + jnp.where(even, cross, same))
    columns = pl.ds(pl.multiple_of(step * width, width), width)
    res_ref[:, columns] = stream_ref[...].astype(F32) + mix

    @pl.when(step == pl.num_programs(0) - 1)
    def _():
        residual = res_ref[...]
        mean = jnp.mean(residual * residual, axis=1, keepdims=True)
        out_ref[...] = (residual * lax.rsqrt(mean + EPS) * gain_ref[...]).astype(BF16)


def hidden_kernel(tiles, x_ref, w_ref, o_ref, buf, sems):
    hidden = w_ref.shape[1] // 2
    copies = []
    for t, (at, size) in enumerate(tiles):
        for part in range(2):
            copy = pltpu.make_async_copy(
                w_ref.at[:, pl.ds(part * hidden + at, size)],
                buf.at[:, pl.ds(part * hidden + at, size)],
                sems.at[t, part],
            )
            copy.start()
            copies.append(copy)
    for t, (at, size) in enumerate(tiles):
        copies[2 * t].wait()
        copies[2 * t + 1].wait()
        gate = dot(x_ref[...], buf[:, at : at + size])
        up = dot(x_ref[...], buf[:, hidden + at : hidden + at + size])
        o_ref[:, at : at + size] = (gate / (1.0 + jnp.exp(-gate)) * up).astype(BF16)


def down_kernel(h_ref, w_ref, o_ref):
    o_ref[...] = dot(h_ref[...], w_ref[...], 1, 1).astype(BF16)


def tiles_of(total, size):
    return [(at, min(size, total - at)) for at in range(0, total, size)]


def state_and_read(qa, ka, qb, kb, v, gate, gain, in_rates, forget_rates, exchange, blocks, halves):
    length = qa.shape[0]
    pieces = sds((blocks, PIECE, LANES), F32)
    held = pltpu.VMEM((3, LANES, LANES), F32)
    own, cum = call(
        state_kernel,
        "state",
        (pieces, sds((8, length), F32)),
        4 * 2 * length * LANES * LANES,
        2 << 20,
        [held],
    )(ka, kb, v, in_rates, forget_rates)
    folded = call(
        fold_kernel,
        "fold",
        pieces,
        1 << 24,
        1 << 20,
        [pltpu.VMEM((blocks, 8, blocks), F32)],
    )(exchange(own))
    before, halves = lax.optimization_barrier((exchange(folded), halves))
    scales = ((LANES // 2) ** -0.5, LANES**-0.5)
    y = call(
        functools.partial(read_kernel, scales),
        "read",
        sds((length, 5 * LANES), BF16),
        4 * 4 * length * length * LANES,
        3 << 20,
        [held],
    )(qa, ka, qb, kb, v, gate, gain, in_rates, cum, before)
    return y, halves


def local(
    stream,
    queries_a,
    keys_a,
    queries_b,
    keys_b,
    values,
    out_gate,
    in_gate,
    forget_gate,
    head_gain,
    out_weight,
    norm_gain,
    gate_weight,
    up_weight,
    down_weight,
):
    tp, sp = lax.axis_size("tp"), lax.axis_size("sp")
    me, core = lax.axis_index("tp"), lax.axis_index("sp") % 2
    length, model = stream.shape
    hidden = gate_weight.shape[1]
    share = length // tp

    both = lax.all_gather(
        jnp.concatenate([gate_weight, up_weight], axis=1), "sp", axis=0, tiled=True
    )
    down = lax.all_gather(jnp.transpose(down_weight), "sp", axis=0, tiled=True)

    half = lax.dynamic_index_in_dim(out_weight, core, 0, keepdims=False)
    mine = [
        lax.ppermute(half, "tp", [((i + d) % tp, i) for i in range(tp)]) for d in range(1, tp)
    ]

    def eight(rates):
        rates = rates.reshape(4, length)
        return jnp.concatenate([rates, rates], axis=0)

    def exchange(pieces):
        return lax.all_to_all(pieces, "sp", 0, 0, tiled=True)

    y, mine = state_and_read(
        queries_a,
        keys_a,
        queries_b,
        keys_b,
        values.reshape(length, -1),
        out_gate.reshape(length, -1),
        head_gain.reshape(1, -1),
        eight(in_gate),
        eight(forget_gate),
        exchange,
        sp,
        mine,
    )
    other = [lax.ppermute(m, "sp", [(i, i ^ 1) for i in range(sp)]) for m in mine]
    y = lax.all_to_all(y.reshape(tp, share, -1), "tp", 0, 0, tiled=True)
    width = 512
    quarter = out_weight.shape[1]
    residual, normed = call(
        project_kernel,
        "project",
        (sds((share, model), F32), sds((share, model), BF16)),
        2 * share * model * model,
        10 << 20,
        grid_spec=pltpu.PrefetchScalarGridSpec(
            num_scalar_prefetch=1,
            grid=(model // width,),
            in_specs=[
                pl.BlockSpec(y.shape, lambda n, s: (0, 0, 0)),
                pl.BlockSpec((2, quarter, width), lambda n, s: (0, 0, n)),
                *([pl.BlockSpec((quarter, width), lambda n, s: (0, n))] * (2 * tp - 2)),
                pl.BlockSpec((share, width), lambda n, s: (s[0], n)),
                pl.BlockSpec((1, model), lambda n, s: (0, 0)),
            ],
            out_specs=[
                pl.BlockSpec((share, model), lambda n, s: (0, 0)),
                pl.BlockSpec((share, model), lambda n, s: (0, 0)),
            ],
        ),
    )(jnp.stack([me, core]).astype(jnp.int32), y, out_weight, *mine, *other, stream, norm_gain[None])
    rows = lax.all_to_all(
        jnp.broadcast_to(normed[None], (tp, share, model)), "tp", 0, 0, tiled=True
    ).reshape(length, model)
    tiles = tiles_of(hidden, 256)
    active = call(
        functools.partial(hidden_kernel, tiles),
        "hidden",
        sds((length, hidden), BF16),
        4 * length * model * hidden,
        16 << 20,
        [pltpu.VMEM((model, 2 * hidden), BF16), pltpu.SemaphoreType.DMA((len(tiles), 2))],
        in_specs=[
            pl.BlockSpec(memory_space=pltpu.VMEM),
            pl.BlockSpec(memory_space=pl.ANY),
        ],
    )(rows, both)
    block = 512
    term = call(
        down_kernel,
        "down",
        sds((length, model), BF16),
        2 * length * model * hidden,
        8 << 20,
        grid=(model // block,),
        in_specs=[
            pl.BlockSpec((length, hidden), lambda n: (0, 0)),
            pl.BlockSpec((block, hidden), lambda n: (n, 0)),
        ],
        out_specs=pl.BlockSpec((length, block), lambda n: (0, n)),
    )(active, down)
    parts = lax.all_to_all(term.reshape(tp, share, model), "tp", 0, 0, tiled=True)
    return (residual + jnp.sum(parts.astype(F32), axis=0)).astype(BF16)


def solution(mesh):
    rows, cols = ("grp", "sp"), "tp"
    return jax.shard_map(
        local,
        mesh=mesh,
        in_specs=(
            P(rows, None),
            P(rows, cols),
            P(rows, cols),
            P(rows, cols),
            P(rows, cols),
            P(rows, None, cols),
            P(rows, None, cols),
            P(None, cols, rows),
            P(None, cols, rows),
            P(None, cols),
            P(None, cols, None),
            P(),
            P("sp", cols),
            P("sp", cols),
            P(cols, "sp"),
        ),
        out_specs=P(("grp", "sp", "tp"), None),
        check_vma=False,
    )
```

```python
import functools

import jax
import jax.numpy as jnp
from jax import lax
from jax.experimental import pallas as pl
from jax.experimental.pallas import tpu as pltpu
from jax.sharding import PartitionSpec as P

F32 = jnp.float32
BF16 = jnp.bfloat16
HIGHEST = lax.Precision.HIGHEST
MESH = pl.DeviceIdType.MESH
EPS = 1e-06
NEG = -1e30
LANES = 128
HALF = LANES // 2
STATE_PIECES = ((0, 8 + HALF), (8 + HALF, HALF), (8 + 2 * HALF, HALF))
STATE_ROWS = 8 + 3 * HALF


def iota(shape, dim):
    return lax.broadcasted_iota(jnp.int32, shape, dim)


def dot(a, b, ca=1, cb=0, precision=None):
    return lax.dot_general(
        a, b, (((ca,), (cb,)), ((), ())), preferred_element_type=F32, precision=precision
    )


def sds(shape, dtype):
    return jax.ShapeDtypeStruct(shape, dtype)


def to_lanes(columns, at):
    row, lane = iota((8, LANES), 0), iota((8, LANES), 1)
    return jnp.sum(jnp.where(lane == row + at, columns, 0.0), axis=0, keepdims=True)


def layer_kernel(cfg, *refs):
    sp, tp, scales, names = cfg
    r = dict(zip(names, refs))
    nz, far = sp // 2, sp // 4
    me, t = lax.axis_index("sp"), lax.axis_index("tp")
    z, c = me // 2, lax.rem(me, 2)
    first_core = c == 0

    def chip(k):
        return lax.rem(z + (k + nz), nz)

    right, left = {"sp": chip(1) * 2 + c}, {"sp": chip(-1) * 2 + c}
    onward = {"sp": jnp.where(first_core, chip(1), chip(-1)) * 2 + c}
    sibling = {"sp": z * 2 + (1 - c)}

    def peer(d):
        return lax.rem(t + d, tp)

    sends = []

    def send(src, dst, send_sem, recv_sem, device):
        copy = pltpu.make_async_remote_copy(
            src_ref=src,
            dst_ref=dst,
            send_sem=send_sem,
            recv_sem=recv_sem,
            device_id=device,
            device_id_type=MESH,
        )
        copy.start()
        sends.append(copy)

    def arrived(dst, send_sem, recv_sem, device):
        pltpu.make_async_remote_copy(
            src_ref=dst,
            dst_ref=dst,
            send_sem=send_sem,
            recv_sem=recv_sem,
            device_id=device,
            device_id_type=MESH,
        ).wait_recv()

    barrier = pltpu.get_barrier_semaphore()
    greeted = [right, left, sibling] + [{"tp": peer(d)} for d in range(1, tp)]
    for device in greeted:
        pl.semaphore_signal(barrier, inc=1, device_id=device, device_id_type=MESH)
    pl.semaphore_wait(barrier, len(greeted))

    def ring(view, own, send_sems, recv_sems, shared):
        def hop(way, s, p, source):
            k = -s if way == 0 else s
            send(
                source if s == 0 else view(k, p),
                view(k, p),
                send_sems.at[way, s, p],
                recv_sems.at[way, s, p],
                right if way == 0 else left,
            )

        def last_hop(p, source):
            k = jnp.where(first_core, chip(1 - far), chip(far - 1))
            send(
                source if far == 1 else view(None, p, k),
                view(None, p, k),
                send_sems.at[0, far - 1, p],
                recv_sems.at[0, far - 1, p],
                onward,
            )

        def step(s, p, source=None):
            if 0 < s < far:
                for way in range(2):
                    k = -s if way == 0 else s
                    arrived(
                        view(k, p),
                        send_sems.at[way, s - 1, p],
                        recv_sems.at[way, s - 1, p],
                        right if way == 0 else left,
                    )
                    if s < far - 1:
                        hop(way, s, p, None)
                    shared(k, p, 2 * s - 1 + way)
                if s == far - 1:
                    last_hop(p, None)
            elif s == 0:
                if far > 1:
                    hop(0, 0, p, source)
                    hop(1, 0, p, source)
                else:
                    last_hop(p, source)
            else:
                arrived(
                    view(far, p),
                    send_sems.at[0, far - 1, p],
                    recv_sems.at[0, far - 1, p],
                    onward,
                )
                shared(far, p, nz - 1)

        return step

    shard_rows, hidden = r["gate_w"].shape
    wall = r["wall"]
    piece_rows = ((0, shard_rows), (0, shard_rows), (0, shard_rows // 2), (shard_rows // 2,) * 2)
    piece_cols = (0, hidden, 2 * hidden, 2 * hidden)

    def weight_view(k, p, at=None, core=None):
        at = chip(k) if at is None else at
        row = (at * 2 + (c if core is None else core)) * shard_rows + piece_rows[p][0]
        row = pl.multiple_of(row, shard_rows // 2)
        return wall.at[pl.ds(row, piece_rows[p][1]), pl.ds(piece_cols[p], hidden)]

    def own_weight(p):
        if p < 2:
            return r["gate_w"] if p == 0 else r["up_w"]
        return r["down_w"].at[pl.ds(piece_rows[p][0], piece_rows[p][1]), :]

    def weight_to_sibling(k, p, n, source=None):
        view = weight_view(k, p)
        send(
            view if source is None else source,
            view,
            r["wb_send"].at[n, p],
            r["wb_recv"].at[n, p],
            sibling,
        )

    weight_step = ring(
        weight_view, own_weight, r["w_send"], r["w_recv"], weight_to_sibling
    )
    for p in range(2):
        weight_step(0, p, own_weight(p))
    local = []
    for p in range(4):
        copy = pltpu.make_async_copy(own_weight(p), weight_view(0, p), r["own_sem"].at[p])
        copy.start()
        local.append(copy)

    ow = r["ow"]
    copy = pltpu.make_async_copy(r["out_w"], ow.at[t], r["own_sem"].at[4])
    copy.start()
    local.append(copy)
    for d in range(1, tp):
        send(
            r["out_w"].at[c],
            ow.at[t, c],
            r["o_send"].at[d - 1],
            r["o_recv"].at[d - 1],
            {"tp": peer(d)},
        )
    for p in range(2):
        weight_to_sibling(0, p, 0, own_weight(p))

    length = r["qa"].shape[0]
    f = r["forget"][...]
    ls = jnp.minimum(f, 0.0) - jnp.log1p(jnp.exp(-jnp.abs(f)))
    upto = (iota((length, length), 0) <= iota((length, length), 1)).astype(F32)
    cum = dot(ls, upto, precision=HIGHEST)
    in_rates = r["in_rates"][...]
    total = cum[:, length - 1 : length]
    tail = total - cum + in_rates
    peak = jnp.max(tail, axis=1, keepdims=True)
    weight = jnp.exp(tail - peak)
    by_row = jnp.transpose(weight)
    head_lane = iota((1, LANES), 1) < HALF
    ka = r["ka"][...]

    def weighted(n):
        v = r["v"][:, n * LANES : (n + 1) * LANES].astype(F32)
        return (v * by_row[:, n : n + 1]).astype(BF16)

    state = r["state"]
    norms = dot(weight, ka.astype(F32), precision=HIGHEST)
    norms = [jnp.where(head_lane, norms[0:1], norms[1:2])]
    state[0, 8 : 8 + LANES, :] = jnp.where(
        head_lane, dot(weighted(0), ka, 0, 0), dot(weighted(1), ka, 0, 0)
    )
    for h in range(2):
        kb = r["kb"][:, h * LANES : (h + 1) * LANES]
        at = 8 + (1 + h) * LANES
        state[0, at : at + LANES, :] = dot(weighted(2 + h), kb, 0, 0)
        norms.append(dot(weight, kb.astype(F32), precision=HIGHEST)[2 + h : 3 + h])
    norms.append(to_lanes(total, 0) + to_lanes(peak, 8))
    norms.append(jnp.zeros((4, LANES), F32))
    state[0, 0:8, :] = jnp.concatenate(norms, axis=0)
    send(state.at[0], state.at[1], r["b_send"].at[0], r["b_recv"].at[0], sibling)
    for p in range(2, 4):
        weight_to_sibling(0, p, 0, own_weight(p))

    rows = 128
    cum_col = jnp.transpose(cum)
    lane_half = iota((rows, LANES), 1) < HALF
    num_ref, den_ref, max_ref = r["num"], r["den"], r["max"]

    def query(n, at):
        if n < 2:
            q = r["qa"][at : at + rows, :]
            return jnp.where(lane_half == (n == 0), q, jnp.zeros_like(q))
        return r["qb"][at : at + rows, (n - 2) * LANES : (n - 1) * LANES]

    def inside(n, at):
        seen = at + rows
        if n < 2:
            k = r["ka"][0:seen, :]
        else:
            k = r["kb"][0:seen, (n - 2) * LANES : (n - 1) * LANES]
        causal = iota((rows, seen), 0) + at >= iota((rows, seen), 1)
        level = cum_col[at : at + rows, n : n + 1] - cum[n : n + 1, 0:seen]
        level = jnp.where(causal, level + in_rates[n : n + 1, 0:seen], -jnp.inf)
        top = jnp.max(level, axis=1, keepdims=True)
        p = dot(query(n, at), k, 1, 1) * scales[n // 2] * jnp.exp(level - top)
        den_ref[n, at : at + rows, :] = jnp.sum(p, axis=1, keepdims=True)
        max_ref[n, at : at + rows, :] = top
        v = r["v"][0:seen, n * LANES : (n + 1) * LANES]
        num_ref[n, at : at + rows, :] = dot(p.astype(BF16), v)

    units = [(n, at) for at in range(0, length, rows) for n in range(4)]

    def attend(count):
        for _ in range(min(count, len(units))):
            inside(*units.pop(0))

    attend(2)

    arrived(state.at[1], r["b_send"].at[0], r["b_recv"].at[0], sibling)
    scal = [jnp.transpose(state[k, 0:8, :])[0:16, 3:4] for k in range(2)]
    early_e = jnp.where(first_core, scal[0][0:8], scal[1][0:8])
    early_a = jnp.where(first_core, scal[0][8:16], scal[1][8:16])
    late_e = jnp.where(first_core, scal[1][0:8], scal[0][0:8])
    late_a = jnp.where(first_core, scal[1][8:16], scal[0][8:16])
    both_a = jnp.maximum(late_e + early_a, late_a)
    early_w = jnp.exp(late_e + early_a - both_a)
    late_w = jnp.exp(late_a - both_a)
    own_w = jnp.where(first_core, early_w, late_w)
    other_w = jnp.where(first_core, late_w, early_w)

    def spread(columns, m):
        if m == 0:
            return jnp.where(head_lane, columns[0:1], columns[1:2])
        return jnp.broadcast_to(columns[1 + m : 2 + m], (1, LANES))

    travel = r["travel"]
    head = []
    for m in range(3):
        wo, ws = spread(own_w, m), spread(other_w, m)
        head.append(wo * state[0, m : m + 1, :] + ws * state[1, m : m + 1, :])
        source = pl.ds(pl.multiple_of(8 + m * LANES + c * HALF, 8), HALF)
        target = slice(8 + m * HALF, 8 + (m + 1) * HALF)
        travel[z, target, :] = wo * state[0, source, :] + ws * state[1, source, :]
    head.append(to_lanes(early_e + late_e, 0) + to_lanes(both_a, 8))
    head.append(jnp.zeros((4, LANES), F32))
    travel[z, 0:8, :] = jnp.concatenate(head, axis=0)

    def state_view(k, p, at=None):
        at = chip(k) if at is None else at
        return travel.at[at, pl.ds(*STATE_PIECES[p]), :]

    state_step = ring(
        state_view, None, r["s_send"], r["s_recv"], lambda k, p, n: None
    )
    for p in range(3):
        state_step(0, p, state_view(0, p))
    for s in range(1, far + 1):
        attend(3)
        for p in range(3):
            state_step(s, p)
    attend(len(units))

    scalars = jnp.concatenate([travel[k, 3:4, :] for k in range(nz)], axis=0)
    if nz < 8:
        scalars = jnp.concatenate([scalars, jnp.zeros((8 - nz, LANES), F32)], axis=0)
    scalars = jnp.transpose(scalars)
    e, a = scalars[0:8], scalars[8:16]
    lane = iota(e.shape, 1)
    gap = jnp.zeros(e.shape, F32)
    for k in range(nz):
        gap = gap + jnp.where((lane < k) & (k < z), e[:, k : k + 1], 0.0)
    level = jnp.where(lane < z, gap + a, -jnp.inf)
    start = jnp.maximum(jnp.max(level, axis=1, keepdims=True), NEG)
    fold = jnp.exp(level - start)
    after = jnp.maximum(early_e + start, early_a)
    keep = jnp.where(first_core, 1.0, jnp.exp(early_e + start - after))
    add = jnp.where(first_core, 0.0, jnp.exp(early_a - after))
    own_start = jnp.where(first_core, start, after)
    carried = r["carried"]
    begun = []
    for m in range(3):
        target = slice(8 + m * HALF, 8 + (m + 1) * HALF)
        acc = jnp.zeros((HALF, LANES), F32)
        norm = jnp.zeros((1, LANES), F32)
        for k in range(nz):
            w = spread(fold[:, k : k + 1], m)
            acc = acc + w * travel[k, target, :]
            norm = norm + w * travel[k, m : m + 1, :]
        carried[c, m] = acc
        begun.append(norm)
    send(carried.at[c], carried.at[c], r["b_send"].at[1], r["b_recv"].at[1], sibling)
    for p in range(2):
        weight_step(1, p)
    arrived(carried.at[1 - c], r["b_send"].at[1], r["b_recv"].at[1], sibling)
    starts = []
    for m in range(3):
        wk, wa = spread(keep, m), spread(add, m)
        at = 8 + m * LANES
        early = jnp.where(first_core, state[0, at : at + LANES, :], state[1, at : at + LANES, :])
        norm = jnp.where(first_core, state[0, m : m + 1, :], state[1, m : m + 1, :])
        whole = jnp.concatenate([carried[0, m], carried[1, m]], axis=0) * wk + wa * early
        high = whole.astype(BF16)
        low = (whole - high.astype(F32)).astype(BF16)
        starts.append((high, low, begun[m] * wk + wa * norm))

    y_own, y_all = r["y_own"], r["y_all"]
    share = length // tp
    for at in range(0, length, rows):
        squares = [jnp.zeros((rows, 1), F32)] * 2
        for n in range(4):
            m = max(n - 1, 0)
            high, low, norm = starts[m]
            q = query(n, at)
            carry = cum_col[at : at + rows, n : n + 1] + own_start[n : n + 1]
            top = max_ref[n, at : at + rows, :]
            peak = jnp.maximum(carry, top)
            scale = jnp.exp(top - peak)
            before = jnp.exp(carry - peak) * scales[n // 2]
            reach = jnp.sum(q.astype(F32) * norm, axis=1, keepdims=True)
            den = scale * den_ref[n, at : at + rows, :] + before * reach
            num = scale * num_ref[n, at : at + rows, :]
            num = num + before * (dot(q, high, 1, 1) + dot(q, low, 1, 1))
            cell = num / jnp.maximum(jnp.abs(den), jnp.exp(-peak))
            squares[n // 2] = squares[n // 2] + jnp.sum(cell * cell, axis=1, keepdims=True)
            columns = slice(n * LANES, (n + 1) * LANES)
            gate = r["out_gate"][at : at + rows, columns].astype(F32)
            y = cell * r["head_gain"][0:1, columns] / (1.0 + jnp.exp(-gate))
            y_own[at : at + rows, columns] = y.astype(BF16)
        lane = iota((rows, LANES), 1)
        extra = jnp.zeros((rows, LANES), F32)
        for group in range(2):
            rest = squares[group]
            for k in range(3):
                piece = rest.astype(BF16).astype(F32)
                extra = jnp.where(lane == 3 * group + k, piece, extra)
                rest = rest - piece
        y_own[at : at + rows, 4 * LANES :] = extra.astype(BF16)

    def rows_of(ref, j, half=None):
        size = share if half is None else share // 2
        at = j * share + (0 if half is None else half * size)
        return ref.at[pl.ds(pl.multiple_of(at, share // 2), size), :]

    for d in range(1, tp):
        send(
            rows_of(y_own, peer(d)),
            y_all.at[t],
            r["y_send"].at[d - 1],
            r["y_recv"].at[d - 1],
            {"tp": peer(d)},
        )
    y_all[t] = y_own[pl.ds(pl.multiple_of(t * share, share), share), :]
    for d in range(1, tp):
        j = peer(tp - d)
        arrived(ow.at[j, c], r["o_send"].at[d - 1], r["o_recv"].at[d - 1], {"tp": j})
        send(ow.at[j, c], ow.at[j, c], r["ob_send"].at[d - 1], r["ob_recv"].at[d - 1], sibling)
    for p in range(2):
        weight_step(2, p) if far >= 2 else None
    for d in range(1, tp):
        j = peer(tp - d)
        arrived(y_all.at[j], r["y_send"].at[d - 1], r["y_recv"].at[d - 1], {"tp": j})
        arrived(ow.at[j, 1 - c], r["ob_send"].at[d - 1], r["ob_recv"].at[d - 1], sibling)
    for copy in local:
        copy.wait()

    model = r["stream"].shape[1]
    quarter = 2 * LANES
    totals = jnp.zeros((share, LANES), F32)
    for j in range(tp):
        totals = totals + y_all[j, :, 4 * LANES :].astype(F32)
    factor = []
    for g in range(2):
        square = jnp.sum(totals[:, 3 * g : 3 * g + 3], axis=1, keepdims=True)
        factor.append(lax.rsqrt(square / (tp * quarter) + EPS))
    own_rows = pl.ds(pl.multiple_of(t * share, share), share)
    width = min(512, model)
    mean = jnp.zeros((share, 1), F32)
    res = r["res"]
    for at in range(0, model, width):
        columns = slice(at, at + width)
        mix = jnp.zeros((share, width), F32)
        for g in range(2):
            acc = jnp.zeros((share, width), F32)
            for j in range(tp):
                acc = acc + dot(y_all[j, :, g * quarter : (g + 1) * quarter], ow[j, g, :, columns])
            mix = mix + factor[g] * acc
        residual = r["stream"][own_rows, columns].astype(F32) + mix
        res[:, columns] = residual
        mean = mean + jnp.sum(residual * residual, axis=1, keepdims=True)
    factor = lax.rsqrt(mean / model + EPS)
    x = r["x"]
    for at in range(0, model, width):
        columns = slice(at, at + width)
        x[own_rows, columns] = (res[:, columns] * factor * r["norm_gain"][0:1, columns]).astype(
            BF16
        )

    to_right, to_left = {"tp": peer(1)}, {"tp": peer(tp - 1)}

    def x_send(j, half, n, device):
        view = rows_of(x, j, half)
        send(view, view, r["x_send"].at[n], r["x_recv"].at[n], device)

    def x_arrived(j, half, n, device):
        arrived(rows_of(x, j, half), r["x_send"].at[n], r["x_recv"].at[n], device)

    x_send(t, 0, 0, to_right)
    x_send(t, 1, 1, to_left)
    x_send(t, 1, 2, to_right)
    x_send(t, 0, 3, to_left)
    for p in range(2):
        weight_step(3, p) if far >= 3 else None
    x_arrived(peer(tp - 1), 0, 0, to_right)
    x_send(peer(tp - 1), 0, 4, to_right)
    x_arrived(peer(1), 1, 1, to_left)
    x_send(peer(1), 1, 5, to_left)
    later = [(s, p) for s in range(4, far + 1) for p in range(2)]
    for s, p in later[0:1]:
        weight_step(s, p)
    x_arrived(peer(tp - 1), 1, 2, to_right)
    x_arrived(peer(1), 0, 3, to_left)
    for s, p in later[1:2]:
        weight_step(s, p)
    x_arrived(peer(2), 0, 4, to_right)
    x_arrived(peer(2), 1, 5, to_left)
    for s, p in later[2:]:
        weight_step(s, p)
    for p in range(2, 4):
        weight_step(0, p, own_weight(p))

    def from_sibling(p):
        for n in range(nz):
            if n == 0:
                k = 0
            elif n == nz - 1:
                k = far
            else:
                k = -((n + 1) // 2) if n % 2 else n // 2
            arrived(
                weight_view(k, p, core=1 - c), r["wb_send"].at[n, p], r["wb_recv"].at[n, p], sibling
            )

    from_sibling(0)
    from_sibling(1)
    h = r["h"]
    tile = 256
    pending = [(s, p) for s in range(1, far + 1) for p in range(2, 4)]
    for at in range(0, hidden, tile):
        size = min(tile, hidden - at)
        gate = dot(x[...], wall[:, at : at + size])
        up = dot(x[...], wall[:, hidden + at : hidden + at + size])
        h[:, at : at + size] = (gate / (1.0 + jnp.exp(-gate)) * up).astype(BF16)
        for s, p in pending[0:1]:
            weight_step(s, p)
        pending = pending[1:]
    for s, p in pending:
        weight_step(s, p)
    from_sibling(2)
    from_sibling(3)

    term, heard = r["term"], r["heard"]
    part = share // 2

    def product(j, half):
        at = pl.multiple_of(j * share + half * part, part)
        return dot(h[pl.ds(at, part), :], wall[:, 2 * hidden : 3 * hidden], 1, 1)

    def hand(slot, n, device):
        send(term.at[slot], heard.at[n], r["t_send"].at[n], r["t_recv"].at[n], device)

    def heard_from(n, device):
        arrived(heard.at[n], r["t_send"].at[n], r["t_recv"].at[n], device)

    term[0] = product(peer(2), 0).astype(BF16)
    hand(0, 0, to_right)
    term[1] = product(peer(2), 1).astype(BF16)
    hand(1, 1, to_left)
    term[2] = product(peer(1), 1).astype(BF16)
    hand(2, 2, to_right)
    term[3] = product(peer(tp - 1), 0).astype(BF16)
    hand(3, 3, to_left)
    kept = product(peer(1), 0)
    heard_from(0, to_right)
    term[4] = (kept + heard[0].astype(F32)).astype(BF16)
    hand(4, 4, to_right)
    kept = product(peer(tp - 1), 1)
    heard_from(1, to_left)
    term[5] = (kept + heard[1].astype(F32)).astype(BF16)
    hand(5, 5, to_left)
    low = res[0:part, :] + product(t, 0)
    high = res[part:, :] + product(t, 1)
    for n in (2, 4):
        heard_from(n, to_right)
    for n in (3, 5):
        heard_from(n, to_left)
    low = low + heard[4].astype(F32) + heard[3].astype(F32)
    high = high + heard[2].astype(F32) + heard[5].astype(F32)
    r["out"][0:part, :] = low.astype(BF16)
    r["out"][part:, :] = high.astype(BF16)
    for copy in sends:
        copy.wait_send()


def local(
    stream,
    queries_a,
    keys_a,
    queries_b,
    keys_b,
    values,
    out_gate,
    in_gate,
    forget_gate,
    head_gain,
    out_weight,
    norm_gain,
    gate_weight,
    up_weight,
    down_weight,
):
    tp, sp = lax.axis_size("tp"), lax.axis_size("sp")
    length, model = stream.shape
    shard_rows, hidden = gate_weight.shape
    share, nz, far = length // tp, sp // 2, sp // 4
    quarter = out_weight.shape[1]

    def eight(rates):
        rates = rates.reshape(4, length)
        return jnp.concatenate([rates, rates], axis=0)

    inputs = {
        "stream": stream,
        "qa": queries_a,
        "ka": keys_a,
        "qb": queries_b,
        "kb": keys_b,
        "v": values.reshape(length, -1),
        "out_gate": out_gate.reshape(length, -1),
        "in_rates": eight(in_gate),
        "forget": eight(forget_gate),
        "head_gain": head_gain.reshape(1, -1),
        "out_w": out_weight,
        "norm_gain": norm_gain[None],
        "gate_w": gate_weight,
        "up_w": up_weight,
        "down_w": jnp.transpose(down_weight),
    }
    dma = pltpu.SemaphoreType.DMA
    scratch = {
        "wall": pltpu.VMEM((sp * shard_rows, 3 * hidden), BF16),
        "ow": pltpu.VMEM((tp, 2, quarter, model), BF16),
        "state": pltpu.VMEM((2, 8 + 3 * LANES, LANES), F32),
        "travel": pltpu.VMEM((nz, STATE_ROWS, LANES), F32),
        "carried": pltpu.VMEM((2, 3, HALF, LANES), F32),
        "num": pltpu.VMEM((4, length, LANES), F32),
        "den": pltpu.VMEM((4, length, 1), F32),
        "max": pltpu.VMEM((4, length, 1), F32),
        "y_own": pltpu.VMEM((length, 5 * LANES), BF16),
        "y_all": pltpu.VMEM((tp, share, 5 * LANES), BF16),
        "res": pltpu.VMEM((share, model), F32),
        "x": pltpu.VMEM((length, model), BF16),
        "h": pltpu.VMEM((length, hidden), BF16),
        "term": pltpu.VMEM((6, share // 2, model), BF16),
        "heard": pltpu.VMEM((6, share // 2, model), BF16),
        "w_send": dma((2, far, 4)),
        "w_recv": dma((2, far, 4)),
        "wb_send": dma((nz, 4)),
        "wb_recv": dma((nz, 4)),
        "own_sem": dma((5,)),
        "o_send": dma((tp - 1,)),
        "o_recv": dma((tp - 1,)),
        "ob_send": dma((tp - 1,)),
        "ob_recv": dma((tp - 1,)),
        "b_send": dma((2,)),
        "b_recv": dma((2,)),
        "s_send": dma((2, far, 3)),
        "s_recv": dma((2, far, 3)),
        "y_send": dma((tp - 1,)),
        "y_recv": dma((tp - 1,)),
        "x_send": dma((6,)),
        "x_recv": dma((6,)),
        "t_send": dma((6,)),
        "t_recv": dma((6,)),
    }
    scales = (HALF**-0.5, LANES**-0.5)
    names = (*inputs, "out", *scratch)
    return pl.pallas_call(
        functools.partial(layer_kernel, (sp, tp, scales, names)),
        name="layer",
        out_shape=sds((share, model), BF16),
        in_specs=[pl.BlockSpec(memory_space=pltpu.VMEM)] * len(inputs),
        out_specs=pl.BlockSpec(memory_space=pltpu.VMEM),
        scratch_shapes=list(scratch.values()),
        compiler_params=pltpu.CompilerParams(
            collective_id=0, has_side_effects=True, vmem_limit_bytes=66_000_000
        ),
    )(*inputs.values())


def solution(mesh):
    rows, cols = ("grp", "sp"), "tp"
    return jax.shard_map(
        local,
        mesh=mesh,
        in_specs=(
            P(rows, None),
            P(rows, cols),
            P(rows, cols),
            P(rows, cols),
            P(rows, cols),
            P(rows, None, cols),
            P(rows, None, cols),
            P(None, cols, rows),
            P(None, cols, rows),
            P(None, cols),
            P(None, cols, None),
            P(),
            P("sp", cols),
            P("sp", cols),
            P(cols, "sp"),
        ),
        out_specs=P(("grp", "sp", "tp"), None),
        check_vma=False,
    )
```
